32 devices in a mesh: rep: 2 (over x), fs: 8 (over z, y), tp: 2 (over core).
Axes of the slice: x: 2, y: 2, z: 4, core: 2. Of those that a mesh axis runs over, the one named last changes fastest.
Arguments:
- resid: bfloat16 [4096, 2048], P(('rep', 'fs'), 'tp'), may hold values from -6 to 6
- norm_gains: float32 [3, 2048], replicated, may hold values from 0.1 to 1.9
- gate_one: bfloat16 [2048, 5632], P('fs', 'tp'), may hold values from -0.125 to 0.125
- up_one: bfloat16 [2048, 5632], P('fs', 'tp'), may hold values from -0.125 to 0.125
- down_one: bfloat16 [5632, 2048], P('tp', 'fs'), may hold values from -0.109375 to 0.109375
- proj_u: bfloat16 [2048, 1024], P('fs', 'tp'), may hold values from -0.125 to 0.125
- proj_v: bfloat16 [2048, 1024], P('fs', 'tp'), may hold values from -0.125 to 0.125
- spatial: bfloat16 [8, 128, 128], P('tp'), may hold values from -0.5 to 0.5
- spatial_bias: float32 [8, 128], P('tp'), may hold values from 0.1 to 1.9
- mix_gain: float32 [1024], P('tp'), may hold values from 0.1 to 1.9
- head_gain: float32 [1024], P('tp'), may hold values from 0.1 to 1.9
- proj_out: bfloat16 [1024, 2048], P('tp', 'fs'), may hold values from -0.25 to 0.25
- gate_two: bfloat16 [2048, 5632], P('fs', 'tp'), may hold values from -0.125 to 0.125
- up_two: bfloat16 [2048, 5632], P('fs', 'tp'), may hold values from -0.125 to 0.125
- down_two: bfloat16 [5632, 2048], P('tp', 'fs'), may hold values from -0.109375 to 0.109375
Outputs:
- layer_out: bfloat16 [4096, 2048], P(('rep', 'fs'), 'tp')
The draws below stay inside these ranges and needn't reach their ends.
All inputs are finite; a program needn't handle non-finite values.
Results may differ from the reference program's by a relative error of at most 0.019.
Values may be sent and summed in bfloat16 or wider, within the bound.
A program may use at most 128 MiB of HBM per device.

```python
import jax
import jax.numpy as jnp
from jax import lax

D = 2048
FF = 5632
HEADS = 8
HEAD_DIM = 128
BLOCK = 128
SPAN = 64
GM = 1024
TOKENS = 4096
N_TP = 2


def raised(entries, stream_key, source, target, shards_of, factor):
    owner, partner = [(jnp.arange(entries.shape[position]) // (entries.shape[position] // shards_of)).reshape([-1 if axis == position else 1 for axis in range(entries.ndim)]) for position in (source, target)]
    chosen = jax.random.permutation(stream_key, shards_of)[partner]
    strong = (owner == chosen) | (owner == (partner + shards_of // 2) % shards_of)
    return jnp.where(strong, factor * entries, entries)


def steps_of(own_key, shape, pieces, low, largest):
    def one(dim, shards_of):
        draws = jax.random.uniform(jax.random.fold_in(jax.random.fold_in(own_key, 6), dim), (shards_of,), jnp.float32, low / len(pieces), largest / len(pieces))
        return jnp.repeat(jnp.exp(draws), shape[dim] // shards_of).reshape((-1,) + (1,) * (len(shape) - dim - 1))

    factor_of = one(*pieces[0])
    for cut in pieces[1:]:
        factor_of = factor_of * one(*cut)
    return factor_of


def centred(rng, shape, deviation, reach, cuts=(), held_as=jnp.bfloat16):
    level = steps_of(rng, shape, cuts, -0.22, 0.18) if cuts else 1.0
    drawn = jax.random.normal(rng, shape, jnp.float32) * deviation * level
    return jnp.minimum(jnp.maximum(drawn, -reach), reach).astype(held_as)


def bell_draw_with(key, extent, deviation, most, shards, heavy, dtype=jnp.bfloat16):
    result = deviation * jax.random.normal(key, extent, jnp.float32)
    if shards:
        result = result * steps_of(key, extent, shards, -0.22, 0.18)
    return jnp.clip(raised(result, jax.random.fold_in(key, 3), *heavy), -most, most).astype(dtype)


def setup_inputs(seed: int = 0) -> dict:
    key_list = jax.random.split(jax.random.key(seed), 16)
    return {
        "resid": centred(key_list[0], (TOKENS, D), 1.0, 6.0, ((0, 16), (1, 2))),
        "norm_gains": jnp.clip(1.0 + 0.18 * jax.random.normal(key_list[1], (3, D), jnp.float32), 0.1, 1.9),
        "gate_one": centred(key_list[2], (D, FF), D ** -0.5, 0.125, ((0, 8), (1, 2))),
        "up_one": centred(key_list[3], (D, FF), D ** -0.5, 0.125, ((0, 8), (1, 2))),
        "down_one": bell_draw_with(key_list[4], (FF, D), FF ** -0.5, 0.109375, ((0, 2), (1, 8)), (0, 1, 8, 2.0)),
        "proj_u": centred(key_list[5], (D, GM), D ** -0.5, 0.125, ((0, 8), (1, 2))),
        "proj_v": centred(key_list[6], (D, GM), D ** -0.5, 0.125, ((0, 8), (1, 2))),
        "spatial": centred(key_list[7], (HEADS, BLOCK, BLOCK), BLOCK ** -0.5, 0.5, ((0, 2),)),
        "spatial_bias": jnp.clip(1.0 + 0.18 * jax.random.normal(key_list[8], (HEADS, BLOCK), jnp.float32), 0.1, 1.9),
        "mix_gain": jnp.clip(1.0 + 0.18 * jax.random.normal(key_list[9], (GM,), jnp.float32), 0.1, 1.9),
        "head_gain": jnp.clip(1.0 + 0.18 * jax.random.normal(key_list[10], (GM,), jnp.float32), 0.1, 1.9),
        "proj_out": bell_draw_with(key_list[11], (GM, D), GM ** -0.5, 0.25, ((0, 2), (1, 8)), (0, 1, 8, 2.0)),
        "gate_two": centred(key_list[12], (D, FF), D ** -0.5, 0.125, ((0, 8), (1, 2))),
        "up_two": centred(key_list[13], (D, FF), D ** -0.5, 0.125, ((0, 8), (1, 2))),
        "down_two": bell_draw_with(key_list[14], (FF, D), FF ** -0.5, 0.109375, ((0, 2), (1, 8)), (0, 1, 8, 2.0)),
    }


def rms_scale(values, gain):
    return values * lax.rsqrt(lax.optimization_barrier(jnp.mean(values * values, axis=-1, keepdims=True)) + 1e-06) * gain

def blockwise_sum(hidden, weight, parts):
    width = hidden.shape[1] // parts
    total = jnp.zeros((hidden.shape[0], weight.shape[1]), jnp.float32)
    for index in range(parts):
        partial_sum = jnp.dot(hidden[:, index * width:(index + 1) * width], weight[index * width:(index + 1) * width], preferred_element_type=jnp.float32)
        rounded = lax.optimization_barrier(partial_sum.astype(jnp.bfloat16))
        total = total + rounded.astype(jnp.float32)
    return total

def feed_forward(stream, gain, gate_weight, up_weight, down_weight):
    normed = rms_scale(stream.astype(jnp.float32), gain).astype(jnp.bfloat16)
    gate = jnp.dot(normed, gate_weight, preferred_element_type=jnp.float32)
    up_part = jnp.dot(normed, up_weight, preferred_element_type=jnp.float32)
    hidden = (jax.nn.silu(gate) * up_part).astype(jnp.bfloat16)
    return blockwise_sum(hidden, down_weight, N_TP)

def reference(resid, norm_gains, gate_one, up_one, down_one, proj_u, proj_v, spatial, spatial_bias, mix_gain, head_gain, proj_out, gate_two, up_two, down_two):
    first = (resid.astype(jnp.float32) + 0.5 * feed_forward(resid, norm_gains[0], gate_one, up_one, down_one)).astype(jnp.bfloat16)
    mnormed = rms_scale(first.astype(jnp.float32), norm_gains[1]).astype(jnp.bfloat16)
    u_part = jnp.dot(mnormed, proj_u, preferred_element_type=jnp.float32)
    v_part = jnp.dot(mnormed, proj_v, preferred_element_type=jnp.float32)
    rows = u_part.shape[0]
    seqs = rows // BLOCK
    gated_u = jax.nn.gelu(u_part).reshape(seqs, BLOCK, HEADS, HEAD_DIM)
    gated_v = jax.nn.gelu(v_part).reshape(seqs, BLOCK, HEADS, HEAD_DIM)
    centre = lax.optimization_barrier(jnp.mean(gated_v, axis=-1, keepdims=True))
    spread = lax.optimization_barrier(jnp.mean(jnp.square(gated_v - centre), axis=-1, keepdims=True))
    vn = ((gated_v - centre) * lax.rsqrt(spread + 1e-05) * mix_gain.reshape(HEADS, HEAD_DIM)).astype(jnp.bfloat16)
    segment = jnp.arange(BLOCK) // SPAN
    causal = segment[:, None] >= segment[None, :]
    masked = jnp.where(causal[None], spatial.astype(jnp.float32), 0.0)
    mixed = jnp.einsum('hts,bshd->bthd', masked, vn.astype(jnp.float32)) + spatial_bias.T[None, :, :, None]
    product = gated_u * mixed
    gated = rms_scale(product, head_gain.reshape(HEADS, HEAD_DIM)).astype(jnp.bfloat16).reshape(rows, HEADS * HEAD_DIM)
    branch = blockwise_sum(gated, proj_out, N_TP)
    second = (first.astype(jnp.float32) + branch).astype(jnp.bfloat16)
    return (second.astype(jnp.float32) + 0.5 * feed_forward(second, norm_gains[2], gate_two, up_two, down_two)).astype(jnp.bfloat16)
```

```python
import functools

import jax
import jax.numpy as jnp
from jax import lax
from jax.experimental import pallas as pl
from jax.experimental.pallas import tpu as pltpu
from jax.sharding import PartitionSpec as P


HEAD_DIM = 128
BLOCK = 128
SPAN = 64


def rms_scale(values, gain):
    return values * lax.rsqrt(jnp.mean(values * values, axis=-1, keepdims=True) + 1e-06) * gain


def normalized(stream, gain):
    whole = lax.all_gather(stream, "tp", axis=1, tiled=True).astype(jnp.float32)
    return rms_scale(whole, gain).astype(jnp.bfloat16)


def accumulate(left, piece):
    return jnp.dot(left, piece, preferred_element_type=jnp.float32)


def folders(normed):

    def single(total, piece, start):
        return accumulate(normed, piece)

    def double(totals, pieces, start):
        return (accumulate(normed, pieces[0]), accumulate(normed, pieces[1]))

    return (single, double)


def ffn_inputs(normed, first_weight, second_weight):
    empty = jnp.zeros((normed.shape[0], first_weight.shape[1]), jnp.float32)
    single, _ = folders(normed)
    result = (
        single(empty, lax.all_gather(first_weight, "fs", axis=0, tiled=True), jnp.int32(0)),
        single(empty, lax.all_gather(second_weight, "fs", axis=0, tiled=True), jnp.int32(0)),
    )
    return result


def mixer_inputs(normed, first_weight, second_weight):
    empty = jnp.zeros((normed.shape[0], first_weight.shape[1]), jnp.float32)
    single, _ = folders(normed)
    result = (
        single(empty, lax.all_gather(first_weight, "fs", axis=0, tiled=True), jnp.int32(0)),
        single(empty, lax.all_gather(second_weight, "fs", axis=0, tiled=True), jnp.int32(0)),
    )
    return result


def mover(count, parts, spread, *refs):
    ins, outs = refs[:count], refs[count : 2 * count]
    send, recv, pass_send, pass_recv, local = refs[2 * count :]
    me, rep = lax.axis_index("fs"), lax.axis_index("rep")
    twin = {"rep": 1 - rep}
    barrier = pltpu.get_barrier_semaphore()
    for step in range(1, parts):
        pl.semaphore_signal(
            barrier, inc=1, device_id={"fs": lax.rem(me + step, parts)},
            device_id_type=pl.DeviceIdType.MESH,
        )
    pl.semaphore_signal(barrier, inc=1, device_id=twin, device_id_type=pl.DeviceIdType.MESH)
    pl.semaphore_wait(barrier, parts)

    def block(a, index):
        return ins[a].at[index] if spread else ins[a].at[0]

    def half(a, which):
        size = outs[a].shape[1] // 2
        return pl.ds(pl.multiple_of(which * size, size), size)

    own = [
        pltpu.make_async_copy(block(a, me), outs[a].at[me], local.at[a]) for a in range(count)
    ]
    for copy in own:
        copy.start()

    def first(step, a):
        peer = lax.rem(me + step, parts)
        return pltpu.make_async_remote_copy(
            src_ref=block(a, peer).at[half(a, rep)],
            dst_ref=outs[a].at[me, half(a, rep)],
            send_sem=send.at[a, step],
            recv_sem=recv.at[a, step],
            device_id={"fs": peer},
            device_id_type=pl.DeviceIdType.MESH,
        )

    def second(step, a):
        source = lax.rem(me + parts - step, parts)
        return pltpu.make_async_remote_copy(
            src_ref=outs[a].at[source, half(a, rep)],
            dst_ref=outs[a].at[source, half(a, rep)],
            send_sem=pass_send.at[a, step],
            recv_sem=pass_recv.at[a, step],
            device_id=twin,
            device_id_type=pl.DeviceIdType.MESH,
        )

    steps = [(step, a) for step in range(1, parts) for a in range(count)]
    for step, a in steps:
        first(step, a).start()
    for step, a in steps:
        first(step, a).wait_recv()
        second(step, a).start()
    for step, a in steps:
        second(step, a).wait_recv()
    for step, a in steps:
        first(step, a).wait_send()
        second(step, a).wait_send()
    for copy in own:
        copy.wait()


def moved(arrays, spread, collective_id):
    parts = lax.axis_size("fs")
    count = len(arrays)
    nbytes = sum(2 * x.size for x in arrays) * (1 if spread else parts)
    pair = pltpu.SemaphoreType.DMA((count, parts))
    return pl.pallas_call(
        functools.partial(mover, count, parts, spread),
        out_shape=[jax.ShapeDtypeStruct((parts,) + x.shape[1:], x.dtype) for x in arrays],
        in_specs=[pl.BlockSpec(memory_space=pl.ANY)] * count,
        out_specs=[pl.BlockSpec(memory_space=pl.ANY)] * count,
        scratch_shapes=[pair, pair, pair, pair, pltpu.SemaphoreType.DMA((count,))],
        compiler_params=pltpu.CompilerParams(
            collective_id=collective_id, has_side_effects=True, vmem_limit_bytes=4 * 2**20
        ),
        cost_estimate=pl.CostEstimate(flops=0, bytes_accessed=40 * nbytes, transcendentals=0),
    )(*arrays)


def unit_weights(weights, collective_id):
    gate_weight, up_weight, down_weight = weights
    parts = lax.axis_size("fs")
    rows, units = gate_weight.shape
    cut = [
        x.reshape(rows, parts, units // parts).transpose(1, 0, 2)
        for x in (gate_weight, up_weight)
    ]
    cut.append(down_weight.reshape(parts, units // parts, rows))
    gate, up_part, down = moved(cut, True, collective_id)
    return (
        gate.reshape(parts * rows, units // parts),
        up_part.reshape(parts * rows, units // parts),
        down.transpose(1, 0, 2).reshape(units // parts, parts * rows),
    )


def mixer_weights(first_weight, second_weight, out_weight, collective_id):
    parts = lax.axis_size("fs")
    rows, units = first_weight.shape
    one, two, out = moved(
        [first_weight[None], second_weight[None], out_weight[None]], False, collective_id
    )
    return (
        one.reshape(parts * rows, units),
        two.reshape(parts * rows, units),
        out.transpose(1, 0, 2).reshape(units, parts * rows),
    )


def feed_forward_by_units(stream, gain, weights):
    rows = lax.all_gather(stream, "fs", axis=0, tiled=True)
    gate_weight, up_weight, down_weight = weights
    normed = normalized(rows, gain)
    hidden = (
        jax.nn.silu(accumulate(normed, gate_weight)) * accumulate(normed, up_weight)
    ).astype(jnp.bfloat16)
    terms = accumulate(hidden, down_weight).astype(jnp.bfloat16)
    mine = lax.psum_scatter(terms, "tp", scatter_dimension=1, tiled=True)
    total = lax.psum_scatter(mine, "fs", scatter_dimension=0, tiled=True)
    return total.astype(jnp.float32), mine


def tokens_move(stream, gate_weight):
    fs = lax.axis_size("fs")
    rows, units = gate_weight.shape
    fits = lax.axis_size("rep") == 2 and units % (32 * fs) == 0 and rows % 32 == 0
    return fits and 2 * stream.size * fs < 3 * gate_weight.size * (fs - 1)


def feed_forward(stream, gain, gate_weight, up_weight, down_weight):
    normed = normalized(stream, gain)
    gate, up_part = ffn_inputs(normed, gate_weight, up_weight)
    hidden = (jax.nn.silu(gate) * up_part).astype(jnp.bfloat16)
    terms = jnp.dot(
        hidden,
        lax.all_gather(down_weight, "fs", axis=1, tiled=True),
        preferred_element_type=jnp.float32,
    )
    return lax.psum_scatter(
        terms.astype(jnp.bfloat16), "tp", scatter_dimension=1, tiled=True
    ).astype(jnp.float32)


def body(
    resid,
    norm_gains,
    gate_one,
    up_one,
    down_one,
    proj_u,
    proj_v,
    spatial,
    spatial_bias,
    mix_gain,
    head_gain,
    proj_out,
    gate_two,
    up_two,
    down_two,
):
    by_units = tokens_move(resid, gate_one)
    if by_units:
        weights = unit_weights((gate_one, up_one, down_one), 1)
        total, mine = feed_forward_by_units(resid, norm_gains[0], weights)
        mine, proj_u, proj_v, proj_out = lax.optimization_barrier(
            (mine, proj_u, proj_v, proj_out)
        )
        proj_u, proj_v, proj_out = mixer_weights(proj_u, proj_v, proj_out, 2)
    else:
        total = feed_forward(resid, norm_gains[0], gate_one, up_one, down_one)
    first = (resid.astype(jnp.float32) + 0.5 * total).astype(jnp.bfloat16)
    mnormed = normalized(first, norm_gains[1])
    if by_units:
        u_part, v_part = accumulate(mnormed, proj_u), accumulate(mnormed, proj_v)
    else:
        u_part, v_part = mixer_inputs(mnormed, proj_u, proj_v)
        proj_out = lax.all_gather(proj_out, "fs", axis=1, tiled=True)
    rows = u_part.shape[0]
    seqs = rows // BLOCK
    local_heads = spatial.shape[0]
    gated_u = jax.nn.gelu(u_part).reshape(seqs, BLOCK, local_heads, HEAD_DIM)
    gated_v = jax.nn.gelu(v_part).reshape(seqs, BLOCK, local_heads, HEAD_DIM)
    centre = jnp.mean(gated_v, axis=-1, keepdims=True)
    spread = jnp.mean(jnp.square(gated_v - centre), axis=-1, keepdims=True)
    vn = (
        (gated_v - centre) * lax.rsqrt(spread + 1e-05) * mix_gain.reshape(local_heads, HEAD_DIM)
    ).astype(jnp.bfloat16)
    segment = jnp.arange(BLOCK) // SPAN
    causal = segment[:, None] >= segment[None, :]
    masked = jnp.where(causal[None], spatial, jnp.zeros_like(spatial))
    mixed = (
        jnp.einsum("hts,bshd->bthd", masked, vn, preferred_element_type=jnp.float32)
        + spatial_bias.T[None, :, :, None]
    )
    product = gated_u * mixed
    gated = (
        rms_scale(product, head_gain.reshape(local_heads, HEAD_DIM))
        .astype(jnp.bfloat16)
        .reshape(rows, local_heads * HEAD_DIM)
    )
    terms = jnp.dot(
        gated,
        proj_out,
        preferred_element_type=jnp.float32,
    )
    branch = lax.psum_scatter(
        terms.astype(jnp.bfloat16), "tp", scatter_dimension=1, tiled=True
    ).astype(jnp.float32)
    second = (first.astype(jnp.float32) + branch).astype(jnp.bfloat16)
    if by_units:
        second, gate_two, up_two, down_two = lax.optimization_barrier(
            (second, gate_two, up_two, down_two)
        )
        weights = unit_weights((gate_two, up_two, down_two), 3)
        total, mine = feed_forward_by_units(second, norm_gains[2], weights)
    else:
        total = feed_forward(second, norm_gains[2], gate_two, up_two, down_two)
    return (second.astype(jnp.float32) + 0.5 * total).astype(jnp.bfloat16)


def solution(mesh):
    return jax.shard_map(
        body,
        mesh=mesh,
        in_specs=(
            P(("rep", "fs"), "tp"),
            P(),
            P("fs", "tp"),
            P("fs", "tp"),
            P("tp", "fs"),
            P("fs", "tp"),
            P("fs", "tp"),
            P("tp", None, None),
            P("tp", None),
            P("tp"),
            P("tp"),
            P("tp", "fs"),
            P("fs", "tp"),
            P("fs", "tp"),
            P("tp", "fs"),
        ),
        out_specs=P(("rep", "fs"), "tp"),
        check_vma=False,
    )
```
